256 devices in a mesh: fs: 32 (over z, x), tp: 8 (over y, core).
Axes of the slice: x: 4, y: 4, z: 8, core: 2. Of those that a mesh axis runs over, the one named last changes fastest.
Arguments:
- saved_input: bfloat16 [81920, 2048], P('fs'), may hold values from -6 to 6
- value_cot: bfloat16 [81920, 1024], P('fs', 'tp'), may hold values from -6 to 6
- query_cot: bfloat16 [81920, 512], P('fs', 'tp'), may hold values from -6 to 6
- value_master: float32 [2048, 1024], P('fs', 'tp'), may hold values from -0.125 to 0.125
- query_master: float32 [2048, 512], P('fs', 'tp'), may hold values from -0.125 to 0.125
- value_factor: bfloat16 [2048, 256], P('fs'), may hold values from -0.125 to 0.125
- query_factor: bfloat16 [2048, 256], P('fs'), may hold values from -0.125 to 0.125
- value_first: float32 [256, 1024], P('fs', 'tp'), as said below
- value_second: float32 [256, 1024], P('fs', 'tp'), as said below
- query_first: float32 [256, 512], P('fs', 'tp'), as said below
- query_second: float32 [256, 512], P('fs', 'tp'), as said below
Outputs:
- value_step: float32 [2048, 1024], P('fs', 'tp')
- query_step: float32 [2048, 512], P('fs', 'tp')
- value_master_new: float32 [2048, 1024], P('fs', 'tp')
- query_master_new: float32 [2048, 512], P('fs', 'tp')
- value_copy: bfloat16 [2048, 1024], P(None, 'tp')
- query_copy: bfloat16 [2048, 512], P(None, 'tp')
- value_first_new: float32 [256, 1024], P('fs', 'tp')
- value_second_new: float32 [256, 1024], P('fs', 'tp')
- query_first_new: float32 [256, 512], P('fs', 'tp')
- query_second_new: float32 [256, 512], P('fs', 'tp')
The draws below stay inside these ranges and needn't reach their ends.
Inputs may be any that keep to these rules, and one draw needn't show every extreme that they name: `value_first`: first moments are real-valued of the projected gradient's order. `value_second`: second moments are positive. `query_first`: first moments are real-valued of the projected gradient's order. `query_second`: second moments are positive.
All inputs are finite; a program needn't handle non-finite values.
Results may differ from the reference program's by a relative error of at most 0.001.
Values may be sent and summed in bfloat16 or wider, within the bound.
A program may use at most 64 MiB of HBM per device.

```python
import jax
import jax.numpy as jnp
from jax import lax

D = 2048
RANK = 256
TOKENS = 81920
V_W = 1024
QK_W = 512


def first_draw(key, width):
    level = 0.1 / jnp.sqrt(jnp.float32(TOKENS))
    values = jax.random.normal(jax.random.fold_in(key, 11), (RANK, width), jnp.float32)
    return values * level


def second_draw(key, width):
    level = 0.05 / jnp.float32(TOKENS)
    row_pos = jnp.arange(RANK, dtype=jnp.float32)[:, None] / RANK
    col_pos = jnp.arange(width, dtype=jnp.float32)[None, :] / width
    spread = jnp.exp(jax.random.uniform(jax.random.fold_in(key, 13), (RANK, width), jnp.float32, -0.7, 0.7))
    rising = 10.0 ** row_pos * 10.0 ** col_pos
    return level * spread * rising


def draw_value_first(key, part):
    return first_draw(key, V_W)


def draw_value_second(key, part):
    return second_draw(key, V_W)


def draw_query_first(key, part):
    return first_draw(key, QK_W)


def draw_query_second(key, part):
    return second_draw(key, QK_W)


def strengthened(entries, own_key, source, target, shards_of, factor):
    owner, partner = [(jnp.arange(entries.shape[axis_at]) // (entries.shape[axis_at] // shards_of)).reshape([-1 if axis == axis_at else 1 for axis in range(entries.ndim)]) for axis_at in (source, target)]
    chosen = jax.random.permutation(own_key, shards_of)[partner]
    strong = (owner == chosen) | (owner == (partner + shards_of // 2) % shards_of)
    return jnp.where(strong, factor * entries, entries)


def steps_of(stream_key, dims, pieces, smallest, top_value):
    factor_of, own = 1.0, jax.random.fold_in(stream_key, 6)
    for position, shards_of in pieces:
        draws = jnp.exp(jax.random.uniform(jax.random.fold_in(own, position), (shards_of,), jnp.float32, smallest / len(pieces), top_value / len(pieces)))
        factor_of = factor_of * jnp.repeat(draws, dims[position] // shards_of).reshape([-1 if axis == position else 1 for axis in range(len(dims))])
    return factor_of


def noise(key, dims, scale, bound, cuts=(), held_as=jnp.bfloat16):
    values = scale * jax.random.normal(key, dims, jnp.float32)
    if cuts:
        values = values * steps_of(key, dims, cuts, -0.22, 0.18)
    return jnp.clip(values, -bound, bound).astype(held_as)


def heavy_noise(rng, dims, scale, bound, shards, heavy, kind=jnp.bfloat16):
    values = scale * jax.random.normal(rng, dims, jnp.float32)
    if shards:
        values = values * steps_of(rng, dims, shards, -0.22, 0.18)
    return jnp.clip(strengthened(values, jax.random.fold_in(rng, 3), *heavy), -bound, bound).astype(kind)


def setup_inputs(seed: int = 0) -> dict:
    arg_keys = jax.random.split(jax.random.key(seed), 12)
    return {
        "saved_input": heavy_noise(arg_keys[0], (TOKENS, D), 1.0, 6.0, ((0, 32),), (0, 1, 32, 2.75)),
        "value_cot": noise(arg_keys[1], (TOKENS, V_W), 1.0, 6.0, ((0, 32), (1, 8))),
        "query_cot": noise(arg_keys[2], (TOKENS, QK_W), 1.0, 6.0, ((0, 32), (1, 8))),
        "value_master": noise(arg_keys[3], (D, V_W), D ** -0.5, 0.125, ((0, 32), (1, 8)), jnp.float32),
        "query_master": noise(arg_keys[4], (D, QK_W), D ** -0.5, 0.125, ((0, 32), (1, 8)), jnp.float32),
        "value_factor": noise(arg_keys[5], (D, RANK), D ** -0.5, 0.125, ((0, 32),)),
        "query_factor": noise(arg_keys[6], (D, RANK), D ** -0.5, 0.125, ((0, 32),)),
        "value_first": draw_value_first(jax.random.fold_in(arg_keys[11], 71), 0),
        "value_second": draw_value_second(jax.random.fold_in(arg_keys[11], 71), 0),
        "query_first": draw_query_first(jax.random.fold_in(arg_keys[11], 71), 0),
        "query_second": draw_query_second(jax.random.fold_in(arg_keys[11], 71), 0),
    }


BETA_ONE = 0.9
BETA_TWO = 0.95
DENOM_EPS = 1e-08
NORM_EPS = 1e-06
STEP_SIZE = 0.05

def moment_update(factor, gradient, first, second):
    projected = jnp.dot(factor.astype(jnp.float32).T, gradient, precision=lax.Precision.HIGHEST)
    first_new = BETA_ONE * first + (1.0 - BETA_ONE) * projected
    second_new = BETA_TWO * second + (1.0 - BETA_TWO) * projected * projected
    direction = first_new / (jnp.sqrt(second_new) + DENOM_EPS)
    return (first_new, second_new, direction)

def reference(saved_input, value_cot, query_cot, value_master, query_master, value_factor, query_factor, value_first, value_second, query_first, query_second):
    value_grad = jnp.dot(saved_input.T, value_cot, preferred_element_type=jnp.float32) / TOKENS
    query_grad = jnp.dot(saved_input.T, query_cot, preferred_element_type=jnp.float32) / TOKENS
    value_first_new, value_second_new, value_direction = moment_update(value_factor, value_grad, value_first, value_second)
    query_first_new, query_second_new, query_direction = moment_update(query_factor, query_grad, query_first, query_second)
    square_sum = jnp.sum(value_direction * value_direction) + jnp.sum(query_direction * query_direction)
    update_scale = 1.0 / jnp.sqrt(square_sum / (RANK * (V_W + QK_W)) + NORM_EPS)
    value_step = jnp.dot(value_factor.astype(jnp.float32), value_direction, precision=lax.Precision.HIGHEST) * update_scale
    query_step = jnp.dot(query_factor.astype(jnp.float32), query_direction, precision=lax.Precision.HIGHEST) * update_scale
    value_master_new = value_master - STEP_SIZE * value_step
    query_master_new = query_master - STEP_SIZE * query_step
    return (value_step, query_step, value_master_new, query_master_new, value_master_new.astype(jnp.bfloat16), query_master_new.astype(jnp.bfloat16), value_first_new, value_second_new, query_first_new, query_second_new)
```

```python
import jax
import jax.numpy as jnp
from jax import lax
from jax.experimental import pallas as pl
from jax.experimental.pallas import tpu as pltpu
from jax.sharding import Mesh
from jax.sharding import PartitionSpec as P

FS = ("z", "x")
TP = ("y", "c")
TOKENS = 81920
BETA_ONE = 0.9
BETA_TWO = 0.95
DENOM_EPS = 1e-08
NORM_EPS = 1e-06
STEP_SIZE = 0.05
ENTRIES = 256 * (1024 + 512)
NZ, NX, NY, NC = 8, 4, 4, 2
SHARDS = NZ * NX
MESH = pl.DeviceIdType.MESH
BLOCKS = 8
BLOCK = 256
F32, BF16 = jnp.float32, jnp.bfloat16


def mod(a, n):
    return lax.rem(a, n)


def ring_distance(d, n):
    return min(d, n - d)


OFFSETS = sorted(
    [(dz, dx) for dz in range(NZ) for dx in range(NX) if dz or dx],
    key=lambda o: -(ring_distance(o[0], NZ) + ring_distance(o[1], NX)),
)


def arrived(ref, sem):
    pltpu.make_async_copy(ref, ref, sem).wait()


def send(src, dst, ssem, rsem, to):
    pltpu.make_async_remote_copy(
        src_ref=src, dst_ref=dst, send_sem=ssem, recv_sem=rsem, device_id=to, device_id_type=MESH
    ).start()


class Gather:
    def __init__(self, buf, recv, sent, z, x, forward=None):
        self.buf, self.recv, self.sent, self.z, self.x, self.forward = buf, recv, sent, z, x, forward

    def at(self, dz, dx):
        owner = mod(self.z + NZ - dz, NZ) * NX + mod(self.x + NX - dx, NX)
        return self.buf.at[owner]

    def put(self, dz, dx, sz, sx):
        block = self.at(dz, dx)
        to = {}
        if sz:
            to["z"] = mod(self.z + NZ + sz, NZ)
        if sx:
            to["x"] = mod(self.x + NX + sx, NX)
        place = ((dz + sz) % NZ) * NX + (dx + sx) % NX
        send(block, block, self.sent, self.recv.at[place], to)

    def take(self, dz, dx):
        block = self.at(dz, dx)
        arrived(block, self.recv.at[dz * NX + dx])
        if self.forward is not None:
            self.forward(block)

    def sent_all(self):
        part = self.buf.at[pl.ds(0, SHARDS - 1)]
        arrived(part, self.sent)


class XThenZ(Gather):
    UP = (4, 4, 3, 3)

    def step(self, s):
        if s == 0:
            for dx in (2, 1, 3):
                self.put(0, 0, 0, dx)
            self.put(0, 0, 1, 0)
            self.put(0, 0, -1, 0)
        elif s == 1:
            for dx in (1, 3, 2):
                self.take(0, dx)
                self.put(0, dx, 1, 0)
                self.put(0, dx, -1, 0)
        else:
            k = s - 1
            for dx in (0, 1, 3, 2):
                up, down = self.UP[dx], 7 - self.UP[dx]
                if k <= up:
                    self.take(k, dx)
                    if k < up:
                        self.put(k, dx, 1, 0)
                if k <= down:
                    self.take(NZ - k, dx)
                    if k < down:
                        self.put(NZ - k, dx, -1, 0)


class ZThenX(Gather):
    WAVES = ((1, 7), (2, 6), (3, 5), (4,))

    def step(self, s):
        if s == 0:
            for dz in (4, 3, 5, 2, 6, 1, 7):
                self.put(0, 0, dz, 0)
            for dx in (2, 1, 3):
                self.put(0, 0, 0, dx)
        elif s <= 4:
            for dz in self.WAVES[s - 1]:
                self.take(dz, 0)
                for dx in (2, 1, 3):
                    self.put(dz, 0, 0, dx)
        else:
            for dz in (0, 1, 7, 2, 6, 3, 5, 4):
                for dx in (1, 3, 2):
                    self.take(dz, dx)


def halves(a):
    hi = a.astype(BF16)
    return hi, (a - hi.astype(F32)).astype(BF16)


def moments(projected, first, second):
    first_new = BETA_ONE * first + (1.0 - BETA_ONE) * projected
    second_new = BETA_TWO * second + (1.0 - BETA_TWO) * projected * projected
    return first_new, second_new, first_new / (jnp.sqrt(second_new) + DENOM_EPS)


def dot(a, b):
    return jnp.dot(a, b, preferred_element_type=F32)


def kernel(
    x_hbm, cv_hbm, cq_hbm, mv_hbm, mq_hbm, fv_hbm, fq_hbm, v1_hbm, v2_hbm, q1_hbm, q2_hbm,
    step_v, step_q, new_v, new_q, copy_v, copy_q, v1_new, v2_new, q1_new, q2_new,
    xb, cv, ct, lv, lq, pv, pq, mb, mq, m1v, m2v, m1q, m2q,
    part, got, dirs, dv, dq, sv, sq, squares,
    in_sem, x_sem, p_recv, m_recv, p_sent, m_sent, d_sent, d_recv, b_sent, b_recv, c_sent, c_recv, s_sent, s_recv,
):
    z, x, y, c = (lax.axis_index(a) for a in ("z", "x", "y", "c"))
    me = z * NX + x
    tp = y * NC + c

    def load(src, dst, i):
        copy = pltpu.make_async_copy(src, dst, in_sem.at[i])
        copy.start()
        return copy

    loads = [
        load(fv_hbm, pv.at[me], 0),
        load(fq_hbm, pq.at[me], 1),
        load(cv_hbm, cv, 2),
        load(cq_hbm, ct.at[pl.ds(128, 64)], 3),
    ]
    x_loads = [
        pltpu.make_async_copy(x_hbm.at[:, pl.ds(BLOCK * j, BLOCK)], xb.at[j], x_sem.at[j]) for j in range(BLOCKS)
    ]
    for copy in x_loads:
        copy.start()
    loads += [
        load(mv_hbm, mb.at[me, pl.ds(0, 64)], 4),
        load(mq_hbm, mq, 5),
        load(v1_hbm, m1v, 6),
        load(v2_hbm, m2v, 7),
        load(q1_hbm, m1q, 8),
        load(q2_hbm, m2q, 9),
    ]

    barrier = pltpu.get_barrier_semaphore()
    greeted = 0
    for dx in range(1, NX):
        pl.semaphore_signal(barrier, inc=1, device_id={"x": mod(x + dx, NX)}, device_id_type=MESH)
        greeted += 1
    for dz in range(1, NZ):
        pl.semaphore_signal(barrier, inc=1, device_id={"z": mod(z + dz, NZ)}, device_id_type=MESH)
        greeted += 1
    tp_peers = []
    for dy in range(NY):
        for dc in range(NC):
            if dy or dc:
                tp_peers.append({"y": mod(y + dy, NY), "c": mod(c + dc, NC)})
    for peer in tp_peers:
        pl.semaphore_signal(barrier, inc=1, device_id=peer, device_id_type=MESH)
        greeted += 1

    partner = {"c": 1 - c}

    def to_partner(block):
        send(block, block, d_sent, d_recv, partner)

    first, second = c == 0, c == 1
    p_x = XThenZ(pv, p_recv, p_sent, z, x, to_partner)
    p_z = ZThenX(pq, p_recv, p_sent, z, x, to_partner)
    m_x = XThenZ(mb, m_recv, m_sent, z, x)
    m_z = ZThenX(mb, m_recv, m_sent, z, x)

    def p_step(*steps):
        @pl.when(first)
        def _():
            for s in steps:
                p_x.step(s)

        @pl.when(second)
        def _():
            for s in steps:
                p_z.step(s)

    def m_step(*steps):
        @pl.when(first)
        def _():
            for s in steps:
                m_z.step(s)

        @pl.when(second)
        def _():
            for s in steps:
                m_x.step(s)

    loads[2].wait()
    loads[3].wait()

    def turn(i, _):
        rows = pl.ds(pl.multiple_of(i * 256, 256), 256)
        ct[pl.ds(0, 128), rows] = cv[rows, :].T
        return ()

    lax.fori_loop(0, 10, turn, ())

    def product(j, _):
        pltpu.make_async_copy(x_hbm.at[:, pl.ds(0, BLOCK)], xb.at[j], x_sem.at[j]).wait()
        g = dot(ct[...], xb[j])
        hi, lo = halves(g)
        lv[j, pl.ds(0, 128), :] = hi[:128]
        lv[j, pl.ds(128, 128), :] = lo[:128]
        lq[j, pl.ds(0, 64), :] = hi[128:]
        lq[j, pl.ds(64, 64), :] = lo[128:]
        return ()

    lax.fori_loop(0, 4, product, ())
    loads[0].wait()
    loads[1].wait()
    pl.semaphore_wait(barrier, greeted)
    p_step(0)
    lax.fori_loop(4, BLOCKS, product, ())
    for copy in loads[4:]:
        copy.wait()
    mb[me, pl.ds(64, 32), :] = jnp.concatenate([mq[pl.ds(0, 32), :], mq[pl.ds(32, 32), :]], axis=1)
    p_step(1, 2, 3)
    p_step(4, 5)
    m_step(0)

    @pl.when(first)
    def _():
        arrived(pq.at[pl.ds(0, SHARDS - 1)], d_recv)

    @pl.when(second)
    def _():
        arrived(pv.at[pl.ds(0, SHARDS - 1)], d_recv)

    def project(j, total):
        tv, tq = total
        slab = pl.ds(pl.multiple_of(4 * j, 4), 4)
        return tv + dot(lv[j], pv[slab].reshape(BLOCK, 256)), tq + dot(lq[j], pq[slab].reshape(BLOCK, 256))

    tv, tq = lax.fori_loop(0, BLOCKS, project, (jnp.zeros((256, 256), F32), jnp.zeros((128, 256), F32)))
    own_v = (tv[:128] + tv[128:]).T
    own_q = tq[:64] + tq[64:]
    own_q = jnp.concatenate([own_q, own_q], axis=0).T
    low = lax.broadcasted_iota(jnp.int32, (4, 128), 1) < 64
    for f in range(SHARDS):
        part[f, 0] = own_v[8 * f : 8 * f + 4]
        part[f, 1] = own_v[8 * f + 4 : 8 * f + 8]
        part[f, 2] = jnp.where(low, own_q[8 * f : 8 * f + 4], own_q[8 * f + 4 : 8 * f + 8])

    for dz, dx in OFFSETS:
        to_z, to_x = mod(z + dz, NZ), mod(x + dx, NX)
        send(part.at[to_z * NX + to_x], got.at[dz * NX + dx - 1], b_sent, b_recv, {"z": to_z, "x": to_x})
    m_step(1)
    arrived(got, b_recv)
    total = (jnp.sum(got[...], axis=0) + part[me]) * (1.0 / TOKENS)
    proj_v = jnp.concatenate([total[0], total[1]], axis=0)
    proj_q = total[2]

    def packed(ref):
        return jnp.concatenate([ref[pl.ds(0, 4), :], ref[pl.ds(4, 4), :]], axis=1)

    a_v, b_v, d_v = moments(proj_v, m1v[...], m2v[...])
    a_q, b_q, d_q = moments(proj_q, packed(m1q), packed(m2q))
    dirs[me, 0] = d_v[:4]
    dirs[me, 1] = d_v[4:]
    dirs[me, 2] = d_q
    v1_new[...] = a_v
    v2_new[...] = b_v
    for ref, val in ((q1_new, a_q), (q2_new, b_q)):
        ref[pl.ds(0, 4), :] = val[:, :64]
        ref[pl.ds(4, 4), :] = val[:, 64:]
    for dz, dx in OFFSETS:
        to_z, to_x = mod(z + dz, NZ), mod(x + dx, NX)
        send(dirs.at[me], dirs.at[me], c_sent, c_recv, {"z": to_z, "x": to_x})
    m_step(2, 3)
    arrived(dirs.at[pl.ds(0, SHARDS - 1)], c_recv)

    all_dirs = dirs[...]
    squares[tp] = jnp.sum(all_dirs * all_dirs, axis=(0, 1))
    for peer in tp_peers:
        send(squares.at[tp], squares.at[tp], s_sent, s_recv, peer)

    for f in range(SHARDS):
        dv[pl.ds(8 * f, 4), :] = dirs[f, 0]
        dv[pl.ds(8 * f + 4, 4), :] = dirs[f, 1]
        dq[pl.ds(8 * f, 4), :] = dirs[f, 2]
        dq[pl.ds(8 * f + 4, 4), :] = pltpu.roll(dirs[f, 2], 64, 1)
    right_v = jnp.concatenate(halves(dv[...]), axis=1)
    right_q = jnp.concatenate(halves(dq[...]), axis=1)

    def steps(j, _):
        slab = pl.ds(pl.multiple_of(4 * j, 4), 4)
        s = dot(pv[slab].reshape(BLOCK, 256), right_v)
        sv[j] = s[:, :128] + s[:, 128:]
        s = dot(pq[slab].reshape(BLOCK, 256), right_q)
        sq[j] = s[:, :128] + s[:, 128:]
        return ()

    lax.fori_loop(0, BLOCKS, steps, ())
    m_step(4, 5)
    arrived(squares.at[pl.ds(0, 7)], s_recv)
    square_sum = jnp.sum(jnp.sum(squares[...], axis=0), keepdims=True)
    scale = 1.0 / jnp.sqrt(square_sum / ENTRIES + NORM_EPS)

    def finish(j, _):
        for i in range(4):
            rows = pl.ds(pl.multiple_of(256 * j + 64 * i, 64), 64)
            master = mb[4 * j + i, pl.ds(0, 64), :]
            copy_v[rows, :] = (master - STEP_SIZE * (sv[j, pl.ds(64 * i, 64), :] * scale)).astype(BF16)
        for i in range(2):
            pair = []
            for k in range(2):
                m = mb[4 * j + 2 * i + k, pl.ds(64, 32), :]
                pair += [m, pltpu.roll(m, 64, 1)]
            master = jnp.concatenate(pair, axis=0)
            new = master - STEP_SIZE * (sq[j, pl.ds(128 * i, 128), :] * scale)
            columns = pl.ds(pl.multiple_of(256 * j + 128 * i, 128), 128)
            copy_q[:, columns] = new.T[:64].astype(BF16)
        return ()

    lax.fori_loop(0, BLOCKS, finish, ())
    mine = pl.ds(pl.multiple_of(64 * x, 64), 64)
    own = sv[z, mine, :] * scale
    step_v[...] = own
    new_v[...] = mb[me, pl.ds(0, 64), :] - STEP_SIZE * own
    own = (sq[z, mine, :] * scale)[:, :64]
    step_q[...] = own
    new_q[...] = mq[...] - STEP_SIZE * own

    p_x.sent_all()
    m_x.sent_all()
    arrived(pv.at[pl.ds(0, SHARDS - 1)], d_sent)
    arrived(got, b_sent)
    arrived(got, c_sent)
    arrived(squares.at[pl.ds(0, 7)], s_sent)


def on_device(
    saved_input, value_cot, query_cot, value_master, query_master, value_factor, query_factor,
    value_first, value_second, query_first, query_second,
):
    vmem = pltpu.VMEM
    dma = pltpu.SemaphoreType.DMA
    shape = jax.ShapeDtypeStruct
    out = pl.pallas_call(
        kernel,
        out_shape=(
            shape((64, 128), F32),
            shape((64, 64), F32),
            shape((64, 128), F32),
            shape((64, 64), F32),
            shape((2048, 128), BF16),
            shape((64, 2048), BF16),
            shape((8, 128), F32),
            shape((8, 128), F32),
            shape((8, 64), F32),
            shape((8, 64), F32),
        ),
        in_specs=[pl.BlockSpec(memory_space=pl.ANY)] * 11,
        out_specs=tuple([pl.BlockSpec(memory_space=pltpu.VMEM)] * 10),
        scratch_shapes=[
            vmem((BLOCKS, 2560, BLOCK), BF16),
            vmem((2560, 128), BF16),
            vmem((192, 2560), BF16),
            vmem((BLOCKS, 256, BLOCK), BF16),
            vmem((BLOCKS, 128, BLOCK), BF16),
            vmem((SHARDS, 64, 256), BF16),
            vmem((SHARDS, 64, 256), BF16),
            vmem((SHARDS, 96, 128), F32),
            vmem((64, 64), F32),
            vmem((8, 128), F32),
            vmem((8, 128), F32),
            vmem((8, 64), F32),
            vmem((8, 64), F32),
            vmem((SHARDS, 3, 4, 128), F32),
            vmem((SHARDS - 1, 3, 4, 128), F32),
            vmem((SHARDS, 3, 4, 128), F32),
            vmem((256, 128), F32),
            vmem((256, 128), F32),
            vmem((BLOCKS, BLOCK, 128), F32),
            vmem((BLOCKS, BLOCK, 128), F32),
            vmem((8, 4, 128), F32),
            dma((10,)),
            dma((BLOCKS,)),
            dma((SHARDS,)),
            dma((SHARDS,)),
            dma,
            dma,
            dma,
            dma,
            dma,
            dma,
            dma,
            dma,
            dma,
            dma,
        ],
        compiler_params=pltpu.CompilerParams(collective_id=0, has_side_effects=True),
        name="moment_update",
    )(
        saved_input, value_cot, query_cot.T, value_master, query_master, value_factor, query_factor,
        value_first, value_second, query_first, query_second,
    )
    step_v, step_q, new_v, new_q, copy_v, copy_q, v1, v2, q1, q2 = out
    return step_v, step_q, new_v, new_q, copy_v, copy_q.T, v1, v2, q1, q2


def solution(mesh):
    split = Mesh(mesh.devices.reshape(NZ, NX, NY, NC), ("z", "x", "y", "c"))
    both = P(FS, TP)
    return jax.shard_map(
        on_device,
        mesh=split,
        in_specs=(P(FS, None), both, both, both, both, P(FS, None), P(FS, None), both, both, both, both),
        out_specs=(both, both, both, both, P(None, TP), P(None, TP), both, both, both, both),
        check_vma=False,
    )
```
